32 devices in a mesh: sp: 8 (over z, y), tp: 4 (over x, core).
Axes of the slice: x: 2, y: 2, z: 4, core: 2. Of those that a mesh axis runs over, the one named last changes fastest.
Arguments:
- residual: bfloat16 [1024, 2048], P(('sp', 'tp')), may hold values from -6 to 6
- query_content: bfloat16 [1024, 1024], P('sp', 'tp'), may hold values from -400 to 400
- query_rotary: bfloat16 [1024, 384], P('sp', 'tp'), may hold values from -16 to 16
- key_latent: bfloat16 [1024, 512], P('sp'), may hold values from -6 to 6
- rotary_key: bfloat16 [1024, 32], P('sp'), may hold values from -6 to 6
- latent_gain: float32 [512], replicated, may hold values from 0.1 to 1.9
- key_weight: bfloat16 [512, 1024], P(None, 'tp'), may hold values from -0.25 to 0.25
- value_weight: bfloat16 [512, 1024], P(None, 'tp'), may hold values from -0.25 to 0.25
- output_gain: float32 [1024], P('tp'), may hold values from 0.1 to 1.9
- output_weight: bfloat16 [1024, 2048], P('tp'), may hold values from -0.1875 to 0.1875
- mixer_gain: float32 [2048], replicated, may hold values from 0.1 to 1.9
- gate_weight: bfloat16 [2048, 5632], P('sp', 'tp'), may hold values from -0.125 to 0.125
- up_weight: bfloat16 [2048, 5632], P('sp', 'tp'), may hold values from -0.125 to 0.125
- down_weight: bfloat16 [5632, 2048], P('tp', 'sp'), may hold values from -0.078125 to 0.078125
Outputs:
- layer_out: bfloat16 [1024, 2048], P(('sp', 'tp'))
The draws below stay inside these ranges and needn't reach their ends.
All inputs are finite; a program needn't handle non-finite values.
Results may differ from the reference program's by a relative error of at most 0.015.
Values may be sent and summed in bfloat16 or wider, within the bound.
A program may use at most 128 MiB of HBM per device.

```python
import math
import jax
import jax.numpy as jnp
from jax import lax

D = 2048
FF = 5632
LATENT = 512
NARROW_HEADS = 8
WIDE_HEADS = 4
NARROW_DIM = 64
WIDE_DIM = 128
ROT_DIM = 32
TOKENS = 1024
CONTENT = 1024
ROTARY = 384
NARROW_DEV = 2
WIDE_DEV = 1
N_TP = 4


def draw_query_content(key, part):
    first_key = jax.random.fold_in(key, 0)
    width = NARROW_HEADS * NARROW_DIM + WIDE_HEADS * WIDE_DIM
    normal = jax.random.normal(first_key, (TOKENS, width), jnp.float32) * 2.5
    return jnp.clip(normal, -20.0, 20.0).astype(jnp.bfloat16)


def levels(stream_key, dims, shards, low, high):
    factor_of = 1.0
    for axis_at, blocks in shards:
        draws = jax.random.uniform(jax.random.fold_in(jax.random.fold_in(stream_key, 6), axis_at), (blocks,), jnp.float32, low / len(shards), high / len(shards))
        factor_of = factor_of * jnp.repeat(jnp.exp(draws), dims[axis_at] // blocks).reshape((-1,) + (1,) * (len(dims) - 1 - axis_at))
    return factor_of


def gaussian(rng, shape, deviation, most, pieces=(), kind=jnp.bfloat16):
    values = deviation * jax.random.normal(rng, shape, jnp.float32)
    if pieces:
        values = values * levels(rng, shape, pieces, -0.22, 0.18)
    return jnp.clip(values, -most, most).astype(kind)


def setup_inputs(seed: int = 0) -> dict:
    streams_of = jax.random.split(jax.random.key(seed), 15)
    residual = gaussian(streams_of[0], (TOKENS, D), 1.0, 6.0, ((0, 32),))
    query_content = draw_query_content(jax.random.fold_in(streams_of[14], 71), 0)
    query_rotary = gaussian(streams_of[2], (TOKENS, ROTARY), 2.5, 16.0, ((0, 8), (1, 4)))
    key_latent = gaussian(streams_of[3], (TOKENS, LATENT), 1.0, 6.0, ((0, 8),))
    rotary_key = gaussian(streams_of[4], (TOKENS, ROT_DIM), 1.0, 6.0, ((0, 8),))
    latent_gain = jnp.clip(1.0 + 0.18 * jax.random.normal(streams_of[5], (LATENT,), jnp.float32), 0.1, 1.9)
    key_weight = gaussian(streams_of[6], (LATENT, CONTENT), LATENT ** -0.5, 0.25, ((1, 4),))
    value_weight = gaussian(streams_of[7], (LATENT, CONTENT), LATENT ** -0.5, 0.25, ((1, 4),))
    output_gain = jnp.clip(1.0 + 0.18 * jax.random.normal(streams_of[8], (CONTENT,), jnp.float32), 0.1, 1.9)
    output_weight = gaussian(streams_of[9], (CONTENT, D), CONTENT ** -0.5, 0.1875, ((0, 4),))
    mixer_gain = jnp.clip(1.0 + 0.18 * jax.random.normal(streams_of[10], (D,), jnp.float32), 0.1, 1.9)
    gate_weight = gaussian(streams_of[11], (D, FF), D ** -0.5, 0.125, ((0, 8), (1, 4)))
    up_weight = gaussian(streams_of[12], (D, FF), D ** -0.5, 0.125, ((0, 8), (1, 4)))
    down_weight = gaussian(streams_of[13], (FF, D), FF ** -0.5, 0.078125, ((0, 4), (1, 8)))
    return {"residual": residual, "query_content": query_content, "query_rotary": query_rotary, "key_latent": key_latent, "rotary_key": rotary_key, "latent_gain": latent_gain, "key_weight": key_weight, "value_weight": value_weight, "output_gain": output_gain, "output_weight": output_weight, "mixer_gain": mixer_gain, "gate_weight": gate_weight, "up_weight": up_weight, "down_weight": down_weight}


epsilon = 1e-06
rope_base = 500000.0

def stored(values):
    return lax.optimization_barrier(values.astype(jnp.bfloat16))

def normalize(values):
    values = values.astype(jnp.float32)
    return values * lax.rsqrt(lax.optimization_barrier(jnp.mean(values * values, axis=-1, keepdims=True)) + epsilon)

def rotate(values, positions):
    half_width = values.shape[-1] // 2
    inverse = 1.0 / jnp.power(rope_base, jnp.arange(0, 2 * half_width, 2, dtype=jnp.float32) / (2 * half_width))
    angles = positions.astype(jnp.float32)[:, None] * inverse[None, :]
    table_shape = (angles.shape[0],) + (1,) * (values.ndim - 2) + (half_width,)
    cosine_table = jnp.cos(angles).reshape(table_shape)
    sine_table = jnp.sin(angles).reshape(table_shape)
    first_half = values[..., :half_width]
    second_half = values[..., half_width:]
    return jnp.concatenate([first_half * cosine_table - second_half * sine_table, second_half * cosine_table + first_half * sine_table], axis=-1)

def split_groups(whole, narrow_size, wide_size):
    row_count = whole.shape[0]
    blocks = whole.reshape(row_count, N_TP, -1)
    narrow_cols = NARROW_DEV * narrow_size
    narrow = blocks[:, :, :narrow_cols].reshape(row_count, N_TP * NARROW_DEV, narrow_size)
    wide = blocks[:, :, narrow_cols:].reshape(row_count, N_TP * WIDE_DEV, wide_size)
    return (narrow, wide)

def join_groups(narrow, wide):
    row_count = narrow.shape[0]
    return jnp.concatenate([narrow.reshape(row_count, N_TP, -1), wide.reshape(row_count, N_TP, -1)], axis=2).reshape(row_count, -1)

def attend(query_part, rotary_part, key_part, rotary_keys, value_part, factor):
    key_float = key_part.astype(jnp.float32)
    rotary_float = rotary_keys.astype(jnp.float32)
    value_float = value_part.astype(jnp.float32)
    row_count = query_part.shape[0]
    block_rows = math.gcd(512, row_count)

    def one_block(offset):
        query_block = lax.dynamic_slice_in_dim(query_part, offset, block_rows, 0).astype(jnp.float32)
        rotary_block = lax.dynamic_slice_in_dim(rotary_part, offset, block_rows, 0).astype(jnp.float32)
        scores = (jnp.einsum('qhd,khd->hqk', query_block, key_float) + jnp.einsum('qhd,kd->hqk', rotary_block, rotary_float)) * factor
        largest = lax.optimization_barrier(jnp.max(scores, axis=-1, keepdims=True))
        powers = jnp.exp(scores - largest)
        totals = lax.optimization_barrier(jnp.sum(powers, axis=-1))
        weights = stored(powers).astype(jnp.float32)
        summed = jnp.einsum('hqk,khd->qhd', weights, value_float)
        return summed / jnp.transpose(totals)[:, :, None]
    offsets = jnp.arange(0, row_count, block_rows, dtype=jnp.int32)
    result = lax.map(one_block, offsets)
    return result.reshape(row_count, result.shape[2], result.shape[3])

def reference(residual, query_content, query_rotary, key_latent, rotary_key, latent_gain, key_weight, value_weight, output_gain, output_weight, mixer_gain, gate_weight, up_weight, down_weight):
    row_count = key_latent.shape[0]
    positions = jnp.arange(row_count, dtype=jnp.int32)
    latent = stored(normalize(key_latent) * latent_gain.astype(jnp.float32))
    key_content = stored(jnp.dot(latent, key_weight, preferred_element_type=jnp.float32))
    value_rows = stored(jnp.dot(latent, value_weight, preferred_element_type=jnp.float32))
    rot_keys = stored(rotate(rotary_key.astype(jnp.float32), positions))
    turned = rotate(query_rotary.astype(jnp.float32).reshape(row_count, -1, ROT_DIM), positions)
    rot_queries = stored(turned).reshape(row_count, -1)
    query_narrow, query_wide = split_groups(query_content, NARROW_DIM, WIDE_DIM)
    rotary_narrow, rotary_wide = split_groups(rot_queries, ROT_DIM, ROT_DIM)
    key_narrow, key_wide = split_groups(key_content, NARROW_DIM, WIDE_DIM)
    value_narrow, value_wide = split_groups(value_rows, NARROW_DIM, WIDE_DIM)
    out_narrow = attend(query_narrow, rotary_narrow, key_narrow, rot_keys, value_narrow, (NARROW_DIM + ROT_DIM) ** (-0.5))
    out_wide = attend(query_wide, rotary_wide, key_wide, rot_keys, value_wide, (WIDE_DIM + ROT_DIM) ** (-0.5))
    mixed = stored(join_groups(normalize(out_narrow), normalize(out_wide)) * output_gain.astype(jnp.float32))
    projected = jnp.dot(mixed, output_weight, preferred_element_type=jnp.float32)
    middle = stored(residual.astype(jnp.float32) + projected)
    normed = stored(normalize(middle) * mixer_gain.astype(jnp.float32))
    gate_sums = jnp.dot(normed, gate_weight, preferred_element_type=jnp.float32)
    up_sums = jnp.dot(normed, up_weight, preferred_element_type=jnp.float32)
    hidden = stored(jax.nn.silu(gate_sums) * up_sums)
    block_width = FF // N_TP
    channel_out = jnp.zeros((row_count, D), jnp.float32)
    for block_index in range(N_TP):
        columns = hidden[:, block_index * block_width:(block_index + 1) * block_width]
        weight_rows = down_weight[block_index * block_width:(block_index + 1) * block_width]
        channel_out = channel_out + stored(jnp.dot(columns, weight_rows, preferred_element_type=jnp.float32)).astype(jnp.float32)
    return (middle.astype(jnp.float32) + channel_out).astype(jnp.bfloat16)
```

```python
import functools

import jax
import jax.numpy as jnp
import numpy as np
from jax import lax
from jax.experimental import pallas as pl
from jax.experimental.pallas import tpu as pltpu
from jax.sharding import PartitionSpec as P

NARROW_HEADS = 8
WIDE_HEADS = 4
NARROW_DIM = 64
WIDE_DIM = 128
ROT_DIM = 32


epsilon = 1e-06
rope_base = 500000.0


def normalize(values):
    values = values.astype(jnp.float32)
    return values * lax.rsqrt(jnp.mean(values * values, axis=-1, keepdims=True) + epsilon)


def rotate(values, positions):
    half_width = values.shape[-1] // 2
    inverse = 1.0 / jnp.power(
        rope_base, jnp.arange(0, 2 * half_width, 2, dtype=jnp.float32) / (2 * half_width)
    )
    angles = positions.astype(jnp.float32)[:, None] * inverse[None, :]
    table_shape = (angles.shape[0],) + (1,) * (values.ndim - 2) + (half_width,)
    cosine_table = jnp.cos(angles).reshape(table_shape)
    sine_table = jnp.sin(angles).reshape(table_shape)
    first_half = values[..., :half_width]
    second_half = values[..., half_width:]
    return jnp.concatenate(
        [
            first_half * cosine_table - second_half * sine_table,
            second_half * cosine_table + first_half * sine_table,
        ],
        axis=-1,
    )


def group_update(carried, query_part, rotary_part, key_part, rotary_keys, value_part, factor):
    running_max, totals, accumulated = carried
    scores = (
        jnp.einsum("qhd,khd->hqk", query_part, key_part, preferred_element_type=jnp.float32)
        + jnp.einsum("qhd,kd->hqk", rotary_part, rotary_keys, preferred_element_type=jnp.float32)
    ) * factor
    new_max = jnp.max(scores, axis=-1)
    shrink = jnp.exp(running_max - new_max)
    powers = jnp.exp(scores - new_max[..., None])
    totals = totals * shrink + jnp.sum(powers, axis=-1)
    added = jnp.einsum(
        "hqk,khd->qhd", powers.astype(jnp.bfloat16), value_part, preferred_element_type=jnp.float32
    )
    accumulated = accumulated * jnp.transpose(shrink)[:, :, None] + added
    return (new_max, totals, accumulated)


def on_device(
    residual,
    query_content,
    query_rotary,
    key_latent,
    rotary_key,
    latent_gain,
    key_weight,
    value_weight,
    output_gain,
    output_weight,
    mixer_gain,
    gate_weight,
    up_weight,
    down_weight,
):
    tp_count = lax.axis_size("tp")
    narrow_dev = NARROW_HEADS // tp_count
    wide_dev = WIDE_HEADS // tp_count
    row_count = key_latent.shape[0]
    positions = lax.axis_index("sp") * row_count + lax.iota(jnp.int32, row_count)
    latent = (normalize(key_latent) * latent_gain).astype(jnp.bfloat16)
    key_rows = jnp.dot(latent, key_weight, preferred_element_type=jnp.float32).astype(jnp.bfloat16)
    value_rows = jnp.dot(latent, value_weight, preferred_element_type=jnp.float32).astype(
        jnp.bfloat16
    )
    rot_keys = rotate(rotary_key.astype(jnp.float32), positions).astype(jnp.bfloat16)
    head_count = narrow_dev + wide_dev
    rot_queries = rotate(
        query_rotary.astype(jnp.float32).reshape(row_count, head_count, ROT_DIM), positions
    ).astype(jnp.bfloat16)
    narrow_cols = narrow_dev * NARROW_DIM
    query_narrow = query_content[:, :narrow_cols].reshape(row_count, narrow_dev, NARROW_DIM)
    query_wide = query_content[:, narrow_cols:].reshape(row_count, wide_dev, WIDE_DIM)
    rotary_narrow = rot_queries[:, :narrow_dev]
    rotary_wide = rot_queries[:, narrow_dev:]
    narrow_factor = (NARROW_DIM + ROT_DIM) ** (-0.5)
    wide_factor = (WIDE_DIM + ROT_DIM) ** (-0.5)

    def start_state(count, width):
        return (
            jnp.full((count, row_count), -jnp.inf, jnp.float32),
            jnp.zeros((count, row_count), jnp.float32),
            jnp.zeros((row_count, count, width), jnp.float32),
        )

    carried = (start_state(narrow_dev, NARROW_DIM), start_state(wide_dev, WIDE_DIM))
    piece_keys = lax.all_gather(key_rows, "sp", axis=0, tiled=True)
    piece_rotary = lax.all_gather(rot_keys, "sp", axis=0, tiled=True)
    piece_values = lax.all_gather(value_rows, "sp", axis=0, tiled=True)
    length = piece_keys.shape[0]
    narrow_keys = piece_keys[:, :narrow_cols].reshape(length, narrow_dev, NARROW_DIM)
    wide_keys = piece_keys[:, narrow_cols:].reshape(length, wide_dev, WIDE_DIM)
    narrow_values = piece_values[:, :narrow_cols].reshape(length, narrow_dev, NARROW_DIM)
    wide_values = piece_values[:, narrow_cols:].reshape(length, wide_dev, WIDE_DIM)
    narrow_state = group_update(
        carried[0],
        query_narrow,
        rotary_narrow,
        narrow_keys,
        piece_rotary,
        narrow_values,
        narrow_factor,
    )
    wide_state = group_update(
        carried[1], query_wide, rotary_wide, wide_keys, piece_rotary, wide_values, wide_factor
    )
    narrow_state, wide_state = (narrow_state, wide_state)

    def finish(carried):
        return normalize(carried[2] / jnp.transpose(carried[1])[:, :, None]).reshape(row_count, -1)

    mixed = (
        jnp.concatenate([finish(narrow_state), finish(wide_state)], axis=1) * output_gain
    ).astype(jnp.bfloat16)
    whole_output = lax.all_gather(output_weight, "tp", axis=0, tiled=True)
    regrouped = lax.all_to_all(mixed, "tp", split_axis=0, concat_axis=1, tiled=True)
    projected = jnp.dot(regrouped, whole_output, preferred_element_type=jnp.float32)
    middle = (residual.astype(jnp.float32) + projected).astype(jnp.bfloat16)
    normed = (normalize(middle) * mixer_gain).astype(jnp.bfloat16)
    block_normed = lax.all_gather(normed, "tp", axis=0, tiled=True)
    gate_sums = jnp.dot(
        block_normed,
        lax.all_gather(gate_weight, "sp", axis=0, tiled=True),
        preferred_element_type=jnp.float32,
    )
    up_sums = jnp.dot(
        block_normed,
        lax.all_gather(up_weight, "sp", axis=0, tiled=True),
        preferred_element_type=jnp.float32,
    )
    down_whole = lax.all_gather(down_weight, "sp", axis=1, tiled=True)
    hidden = (jax.nn.silu(gate_sums) * up_sums).astype(jnp.bfloat16)
    channel_out = lax.psum_scatter(
        jnp.dot(hidden, down_whole, preferred_element_type=jnp.float32).astype(jnp.bfloat16),
        "tp",
        scatter_dimension=0,
        tiled=True,
    ).astype(jnp.float32)
    return (middle.astype(jnp.float32) + channel_out).astype(jnp.bfloat16)


MESH = pl.DeviceIdType.MESH
LANES = 128
PAIR = 2
CHUNKS = 4


def kernel(
    n_sp,
    query_ref,
    turn_ref,
    latent_ref,
    rotary_ref,
    latent_gain_ref,
    key_weight_ref,
    value_weight_ref,
    output_gain_ref,
    mixer_gain_ref,
    cos_ref,
    sin_ref,
    swap_ref,
    residual_ref,
    output_weight_ref,
    gate_ref,
    up_ref,
    down_ref,
    out_ref,
    lat_all,
    rot_all,
    keys,
    values,
    res_all,
    out_all,
    mix_all,
    middle,
    normed,
    gate_all,
    up_all,
    down_all,
    hidden,
    part,
    from_core,
    to_x,
    from_x,
    to_z,
    from_z,
    send_sems,
    recv_sems,
    local_sems,
):
    n_z = n_sp // PAIR
    s = lax.axis_index("sp")
    t = lax.axis_index("tp")
    z, y = s // PAIR, lax.rem(s, PAIR)
    x, c = t // PAIR, lax.rem(t, PAIR)
    rows, depth = latent_ref.shape
    half = rows // PAIR
    sibling = (s, x * PAIR + 1 - c)
    across = (s, (1 - x) * PAIR + c)
    beside = (z * PAIR + 1 - y, t)
    f32 = jnp.float32

    def z_id(step):
        return (lax.rem(z + step, n_z) * PAIR + y, t)

    barrier = pltpu.get_barrier_semaphore()
    greeted = [(lax.rem(s + k, n_sp), t) for k in range(1, n_sp)] + [sibling, across]
    for device in greeted:
        pl.semaphore_signal(barrier, inc=1, device_id=device, device_id_type=MESH)

    used = [0]
    locals_used = [0]
    sent = []

    def local(src, dst):
        copy = pltpu.make_async_copy(src, dst, local_sems.at[locals_used[0]])
        locals_used[0] += 1
        copy.start()
        return copy

    def send(src, dst, device):
        copy = pltpu.make_async_remote_copy(
            src_ref=src,
            dst_ref=dst,
            send_sem=send_sems.at[used[0]],
            recv_sem=recv_sems.at[used[0]],
            device_id=device,
            device_id_type=MESH,
        )
        used[0] += 1
        copy.start()
        sent.append(copy)
        return copy

    width = gate_all.shape[1]
    total_width = gate_ref.shape[1]
    slab = gate_ref.shape[0]

    def first(piece):
        return pl.multiple_of(jnp.minimum(piece * width, total_width - width), LANES)

    def span(owner):
        return pl.ds(pl.multiple_of(owner * slab, slab), slab)

    mine = span(s)
    my_piece = pl.ds(first(z), width)
    half_rows = pl.ds(pl.multiple_of(c * half, half), half)
    locals_first = [
        local(latent_ref, lat_all.at[pl.ds(pl.multiple_of(s * rows, rows), rows)]),
        local(rotary_ref, rot_all.at[pl.ds(pl.multiple_of(s * rows, rows), rows)]),
    ]
    locals_rest = [
        local(residual_ref, res_all.at[x, c, z]),
        local(output_weight_ref, out_all.at[x, c]),
        local(gate_ref.at[:, my_piece], gate_all.at[mine]),
        local(up_ref.at[:, my_piece], up_all.at[mine]),
        local(down_ref.at[my_piece], down_all.at[:, mine]),
    ]
    pl.semaphore_wait(barrier, len(greeted))

    def token_half(owner):
        return pl.ds(pl.multiple_of(owner * rows + c * half, half), half)

    def send_latent(step):
        device = (lax.rem(s + step, n_sp), t)
        return (
            send(latent_ref.at[half_rows], lat_all.at[token_half(s)], device),
            send(rotary_ref.at[half_rows], rot_all.at[token_half(s)], device),
        )

    latent_copies = [send_latent(k) for k in range(1, n_sp)]
    weight_x = send(output_weight_ref, out_all.at[x, c], across)
    residual_z = [send(residual_ref, res_all.at[x, c, z], z_id(k)) for k in range(1, n_z)]
    weight_y = [
        send(gate_ref.at[:, my_piece], gate_all.at[mine], beside),
        send(up_ref.at[:, my_piece], up_all.at[mine], beside),
        send(down_ref.at[my_piece], down_all.at[:, mine], beside),
    ]

    latent_core = []
    for step in range(1, n_sp):
        for copy in latent_copies[step - 1]:
            copy.wait_recv()
        place = token_half(lax.rem(s + n_sp - step, n_sp))
        latent_core.append(send(lat_all.at[place], lat_all.at[place], sibling))
        latent_core.append(send(rot_all.at[place], rot_all.at[place], sibling))
    weight_core = send(output_weight_ref, out_all.at[x, c], sibling)
    for copy in locals_first:
        copy.wait()
    for copy in latent_core:
        copy.wait_recv()

    gain = latent_gain_ref[...]

    def project(block, _):
        place = pl.ds(pl.multiple_of(block * rows, rows), rows)
        raw = lat_all[place, :].astype(f32)
        scale = lax.rsqrt(jnp.mean(raw * raw, axis=-1, keepdims=True) + epsilon)
        latent = (raw * scale * gain).astype(jnp.bfloat16)
        keys[place, :] = jnp.dot(latent, key_weight_ref[...], preferred_element_type=f32).astype(
            jnp.bfloat16
        )
        values[place, :] = jnp.dot(
            latent, value_weight_ref[...], preferred_element_type=f32
        ).astype(jnp.bfloat16)
        return 0

    lax.fori_loop(0, n_sp, project, 0)
    rot_width = rot_all.shape[1]
    rot_raw = rot_all[...]
    swap = swap_ref[...]
    rot_swapped = jnp.dot(rot_raw, swap[:rot_width, :rot_width], preferred_element_type=f32)
    rot_keys = (
        rot_raw.astype(f32) * cos_ref[:, :rot_width] + rot_swapped * sin_ref[:, :rot_width]
    ).astype(jnp.bfloat16)
    here = pl.ds(pl.multiple_of(s * rows, rows), rows)
    turn_raw = turn_ref[...]
    turn_swapped = jnp.dot(turn_raw, swap, preferred_element_type=f32)
    turned = (turn_raw.astype(f32) * cos_ref[here, :] + turn_swapped * sin_ref[here, :]).astype(
        jnp.bfloat16
    )

    content = query_ref.shape[1]
    head_count = turn_ref.shape[1] // rot_width
    wide_dev = (content - head_count * NARROW_DIM) // (WIDE_DIM - NARROW_DIM)
    sizes = [NARROW_DIM] * (head_count - wide_dev) + [WIDE_DIM] * wide_dev
    contract = (((1,), (1,)), ((), ()))
    heads = []
    start = 0
    for index, size in enumerate(sizes):
        cols = slice(start, start + size)
        scores = lax.dot_general(
            query_ref[:, cols], keys[:, cols], contract, preferred_element_type=f32
        )
        scores = scores + lax.dot_general(
            turned[:, index * rot_width : (index + 1) * rot_width],
            rot_keys,
            contract,
            preferred_element_type=f32,
        )
        scores = scores * (size + ROT_DIM) ** (-0.5)
        powers = jnp.exp(scores - jnp.max(scores, axis=-1, keepdims=True))
        totals = jnp.sum(powers, axis=-1, keepdims=True)
        summed = jnp.dot(
            powers.astype(jnp.bfloat16), values[:, cols], preferred_element_type=f32
        )
        attended = summed / totals
        scale = lax.rsqrt(jnp.mean(attended * attended, axis=-1, keepdims=True) + epsilon)
        heads.append(attended * scale)
        start += size
    mixed = (jnp.concatenate(heads, axis=1) * output_gain_ref[...]).astype(jnp.bfloat16)
    mix_all[x, c, z] = mixed

    mix_z = [send(mix_all.at[x, c, z], mix_all.at[x, c, z], z_id(k)) for k in range(1, n_z)]

    def piece_of(step):
        return pl.ds(first(lax.rem(z + step, n_z)), width)

    gate_z = [
        send(gate_ref.at[:, piece_of(k)], gate_all.at[mine], z_id(k)) for k in range(1, n_z)
    ]
    up_z = [send(up_ref.at[:, piece_of(k)], up_all.at[mine], z_id(k)) for k in range(1, n_z)]
    down_z = [
        send(down_ref.at[piece_of(k)], down_all.at[:, mine], z_id(k)) for k in range(1, n_z)
    ]

    for copy in residual_z:
        copy.wait_recv()
    for copy in locals_rest:
        copy.wait()
    residual_x = send(res_all.at[x, c], res_all.at[x, c], across)
    for copy in mix_z:
        copy.wait_recv()
    mix_x = send(mix_all.at[x, c], mix_all.at[x, c], across)
    mix_core = send(mix_all.at[x, c], mix_all.at[x, c], sibling)
    residual_core = send(res_all.at[x, c], res_all.at[x, c], sibling)
    weight_x.wait_recv()
    weight_far = send(out_all.at[1 - x, c], out_all.at[1 - x, c], sibling)
    mix_x.wait_recv()
    mix_far = send(mix_all.at[1 - x, c], mix_all.at[1 - x, c], sibling)
    residual_x.wait_recv()
    residual_far = send(res_all.at[1 - x, c], res_all.at[1 - x, c], sibling)

    def relay(copies, buffer, columns):
        passed = []
        for step in range(1, n_z):
            copies[step - 1].wait_recv()
            place = span(lax.rem(z + n_z - step, n_z) * PAIR + y)
            block = buffer.at[:, place] if columns else buffer.at[place]
            passed.append(send(block, block, beside))
        return passed

    for copy in (weight_core, weight_far, mix_core, mix_far, residual_core, residual_far):
        copy.wait_recv()

    mixer_gain = mixer_gain_ref[...]
    d_model = middle.shape[1]

    def finish_rows(block, _):
        place = pl.ds(pl.multiple_of(block * rows, rows), rows)
        total = res_all[:, :, block].reshape(rows, d_model).astype(f32)
        projected = jnp.zeros((rows, d_model), f32)
        for far in range(PAIR):
            for core in range(PAIR):
                projected = projected + jnp.dot(
                    mix_all[far, core, block], out_all[far, core], preferred_element_type=f32
                )
        mid = (total + projected).astype(jnp.bfloat16)
        middle[place, :] = mid
        wide = mid.astype(f32)
        scale = lax.rsqrt(jnp.mean(wide * wide, axis=-1, keepdims=True) + epsilon)
        normed[place, :] = (wide * scale * mixer_gain).astype(jnp.bfloat16)
        return 0

    lax.fori_loop(0, n_z, finish_rows, 0)

    gate_y = relay(gate_z, gate_all, False)
    up_y = relay(up_z, up_all, False)
    down_y = relay(down_z, down_all, True)
    for copy in gate_y + up_y + weight_y[:2]:
        copy.wait_recv()

    lane = lax.broadcasted_iota(jnp.int32, (rows, width), 1)
    fresh = lane + first(z) >= z * width

    def units(block, _):
        place = pl.ds(pl.multiple_of(block * rows, rows), rows)
        left = normed[place, :]
        gates = jnp.dot(left, gate_all[...], preferred_element_type=f32)
        ups = jnp.dot(left, up_all[...], preferred_element_type=f32)
        value = gates / (1.0 + jnp.exp(-gates)) * ups
        hidden[place, :] = jnp.where(fresh, value, 0.0).astype(jnp.bfloat16)
        return 0

    lax.fori_loop(0, n_z, units, 0)
    for copy in down_y + weight_y[2:]:
        copy.wait_recv()

    chunk = part.shape[-1]
    core_copies = []
    for n in range(CHUNKS):
        product = jnp.dot(
            hidden[...], down_all[:, n * chunk : (n + 1) * chunk], preferred_element_type=f32
        )
        part[n] = product.astype(jnp.bfloat16).reshape(part.shape[1:])
        core_copies.append(send(part.at[n, :, :, 1 - c], from_core.at[n], sibling))
    x_copies = []
    for n in range(CHUNKS):
        core_copies[n].wait_recv()
        to_x[n] = (part[n, :, :, c].astype(f32) + from_core[n].astype(f32)).astype(jnp.bfloat16)
        x_copies.append(send(to_x.at[n, :, 1 - x], from_x.at[n], across))
    z_copies = []
    for n in range(CHUNKS):
        x_copies[n].wait_recv()
        to_z[n] = (to_x[n, :, x].astype(f32) + from_x[n].astype(f32)).astype(jnp.bfloat16)
        z_copies.append(
            [
                send(to_z.at[n, lax.rem(z + k, n_z)], from_z.at[n, k - 1], z_id(k))
                for k in range(1, n_z)
            ]
        )
    strip = out_ref.shape[0]
    own = pl.ds(pl.multiple_of(z * rows + t * strip, strip), strip)
    for n in range(CHUNKS):
        total = to_z[n, z].astype(f32)
        for k in range(1, n_z):
            z_copies[n][k - 1].wait_recv()
            total = total + from_z[n, k - 1].astype(f32)
        cols = slice(n * chunk, (n + 1) * chunk)
        out_ref[:, cols] = (middle[own, cols].astype(f32) + total).astype(jnp.bfloat16)
    for copy in sent:
        copy.wait_send()


def fused(
    n_sp,
    residual,
    query_content,
    query_rotary,
    key_latent,
    rotary_key,
    latent_gain,
    key_weight,
    value_weight,
    output_gain,
    output_weight,
    mixer_gain,
    gate_weight,
    up_weight,
    down_weight,
):
    n_z = n_sp // PAIR
    rows, latent_width = key_latent.shape
    strip, d_model = residual.shape
    tokens = rows * n_sp
    content = query_content.shape[1]
    turn_width = query_rotary.shape[1]
    half_width = ROT_DIM // 2
    inverse = np.float32(1.0) / np.power(
        np.float32(rope_base), np.arange(0, ROT_DIM, 2, dtype=np.float32) / np.float32(ROT_DIM)
    )
    angles = np.arange(tokens, dtype=np.float32)[:, None] * inverse[None, :].astype(np.float32)
    head_count = turn_width // ROT_DIM
    cosine = np.cos(angles).astype(np.float32)
    sine = np.sin(angles).astype(np.float32)
    cos_table = np.tile(np.concatenate([cosine, cosine], axis=1), (1, head_count))
    sin_table = np.tile(np.concatenate([-sine, sine], axis=1), (1, head_count))
    lane = np.arange(turn_width)
    other = lane // ROT_DIM * ROT_DIM + (lane + half_width) % ROT_DIM
    swap = np.zeros((turn_width, turn_width), np.float32)
    swap[other, lane] = 1.0
    tiles = gate_weight.shape[1] // LANES
    width = -(-tiles // n_z) * LANES
    slab = rows * n_z
    chunk = d_model // CHUNKS
    bf16 = jnp.bfloat16
    n_copies = 2 * 2 * (n_sp - 1) + 8 * (n_z - 1) + 16 + CHUNKS * (n_z + 1)
    vmem = pl.BlockSpec(memory_space=pltpu.VMEM)
    anywhere = pl.BlockSpec(memory_space=pl.ANY)
    return pl.pallas_call(
        functools.partial(kernel, n_sp),
        out_shape=jax.ShapeDtypeStruct((strip, d_model), bf16),
        in_specs=[vmem] * 12 + [anywhere] * 5,
        out_specs=vmem,
        scratch_shapes=[
            pltpu.VMEM((tokens, latent_width), bf16),
            pltpu.VMEM((tokens, ROT_DIM), bf16),
            pltpu.VMEM((tokens, content), bf16),
            pltpu.VMEM((tokens, content), bf16),
            pltpu.VMEM((PAIR, PAIR, n_z, strip, d_model), bf16),
            pltpu.VMEM((PAIR, PAIR, content, d_model), bf16),
            pltpu.VMEM((PAIR, PAIR, n_z, rows, content), bf16),
            pltpu.VMEM((slab, d_model), bf16),
            pltpu.VMEM((slab, d_model), bf16),
            pltpu.VMEM((d_model, width), bf16),
            pltpu.VMEM((d_model, width), bf16),
            pltpu.VMEM((width, d_model), bf16),
            pltpu.VMEM((slab, width), bf16),
            pltpu.VMEM((CHUNKS, n_z, PAIR, PAIR, strip, chunk), bf16),
            pltpu.VMEM((CHUNKS, n_z, PAIR, strip, chunk), bf16),
            pltpu.VMEM((CHUNKS, n_z, PAIR, strip, chunk), bf16),
            pltpu.VMEM((CHUNKS, n_z, strip, chunk), bf16),
            pltpu.VMEM((CHUNKS, n_z, strip, chunk), bf16),
            pltpu.VMEM((CHUNKS, n_z - 1, strip, chunk), bf16),
            pltpu.SemaphoreType.DMA((n_copies,)),
            pltpu.SemaphoreType.DMA((n_copies,)),
            pltpu.SemaphoreType.DMA((8,)),
        ],
        compiler_params=pltpu.CompilerParams(
            collective_id=0, has_side_effects=True, vmem_limit_bytes=60 * 1024 * 1024
        ),
        name="layer",
    )(
        query_content,
        query_rotary,
        key_latent,
        rotary_key,
        latent_gain.reshape(1, -1),
        key_weight,
        value_weight,
        output_gain.reshape(1, -1),
        mixer_gain.reshape(1, -1),
        jnp.asarray(cos_table),
        jnp.asarray(sin_table),
        jnp.asarray(swap, dtype=bf16),
        residual,
        output_weight,
        gate_weight,
        up_weight,
        down_weight,
    )


def solution(mesh):
    n_sp, n_tp = mesh.shape["sp"], mesh.shape["tp"]

    def program(*arrays):
        residual, gate_weight = arrays[0], arrays[11]
        fits = (
            n_tp == PAIR * PAIR
            and n_sp % PAIR == 0
            and gate_weight.shape[0] % LANES == 0
            and gate_weight.shape[1] % LANES == 0
            and residual.shape[1] % (CHUNKS * LANES) == 0
        )
        if fits:
            return fused(n_sp, *arrays)
        return on_device(*arrays)

    placed = (
        P(("sp", "tp"), None),
        P("sp", "tp"),
        P("sp", "tp"),
        P("sp", None),
        P("sp", None),
        P(),
        P(None, "tp"),
        P(None, "tp"),
        P("tp"),
        P("tp", None),
        P(),
        P("sp", "tp"),
        P("sp", "tp"),
        P("tp", "sp"),
    )
    return jax.shard_map(
        program, mesh=mesh, in_specs=placed, out_specs=P(("sp", "tp"), None), check_vma=False
    )
```

```python
import functools

import jax
import jax.numpy as jnp
import numpy as np
from jax import lax
from jax.experimental import pallas as pl
from jax.experimental.pallas import tpu as pltpu
from jax.sharding import PartitionSpec as P

NARROW_HEADS = 8
WIDE_HEADS = 4
NARROW_DIM = 64
WIDE_DIM = 128
ROT_DIM = 32


epsilon = 1e-06
rope_base = 500000.0


def normalize(values):
    values = values.astype(jnp.float32)
    return values * lax.rsqrt(jnp.mean(values * values, axis=-1, keepdims=True) + epsilon)


def rotate(values, positions):
    half_width = values.shape[-1] // 2
    inverse = 1.0 / jnp.power(
        rope_base, jnp.arange(0, 2 * half_width, 2, dtype=jnp.float32) / (2 * half_width)
    )
    angles = positions.astype(jnp.float32)[:, None] * inverse[None, :]
    table_shape = (angles.shape[0],) + (1,) * (values.ndim - 2) + (half_width,)
    cosine_table = jnp.cos(angles).reshape(table_shape)
    sine_table = jnp.sin(angles).reshape(table_shape)
    first_half = values[..., :half_width]
    second_half = values[..., half_width:]
    return jnp.concatenate(
        [
            first_half * cosine_table - second_half * sine_table,
            second_half * cosine_table + first_half * sine_table,
        ],
        axis=-1,
    )


def group_update(carried, query_part, rotary_part, key_part, rotary_keys, value_part, factor):
    running_max, totals, accumulated = carried
    scores = (
        jnp.einsum("qhd,khd->hqk", query_part, key_part, preferred_element_type=jnp.float32)
        + jnp.einsum("qhd,kd->hqk", rotary_part, rotary_keys, preferred_element_type=jnp.float32)
    ) * factor
    new_max = jnp.max(scores, axis=-1)
    shrink = jnp.exp(running_max - new_max)
    powers = jnp.exp(scores - new_max[..., None])
    totals = totals * shrink + jnp.sum(powers, axis=-1)
    added = jnp.einsum(
        "hqk,khd->qhd", powers.astype(jnp.bfloat16), value_part, preferred_element_type=jnp.float32
    )
    accumulated = accumulated * jnp.transpose(shrink)[:, :, None] + added
    return (new_max, totals, accumulated)


def on_device(
    residual,
    query_content,
    query_rotary,
    key_latent,
    rotary_key,
    latent_gain,
    key_weight,
    value_weight,
    output_gain,
    output_weight,
    mixer_gain,
    gate_weight,
    up_weight,
    down_weight,
):
    tp_count = lax.axis_size("tp")
    narrow_dev = NARROW_HEADS // tp_count
    wide_dev = WIDE_HEADS // tp_count
    row_count = key_latent.shape[0]
    positions = lax.axis_index("sp") * row_count + lax.iota(jnp.int32, row_count)
    latent = (normalize(key_latent) * latent_gain).astype(jnp.bfloat16)
    key_rows = jnp.dot(latent, key_weight, preferred_element_type=jnp.float32).astype(jnp.bfloat16)
    value_rows = jnp.dot(latent, value_weight, preferred_element_type=jnp.float32).astype(
        jnp.bfloat16
    )
    rot_keys = rotate(rotary_key.astype(jnp.float32), positions).astype(jnp.bfloat16)
    head_count = narrow_dev + wide_dev
    rot_queries = rotate(
        query_rotary.astype(jnp.float32).reshape(row_count, head_count, ROT_DIM), positions
    ).astype(jnp.bfloat16)
    narrow_cols = narrow_dev * NARROW_DIM
    query_narrow = query_content[:, :narrow_cols].reshape(row_count, narrow_dev, NARROW_DIM)
    query_wide = query_content[:, narrow_cols:].reshape(row_count, wide_dev, WIDE_DIM)
    rotary_narrow = rot_queries[:, :narrow_dev]
    rotary_wide = rot_queries[:, narrow_dev:]
    narrow_factor = (NARROW_DIM + ROT_DIM) ** (-0.5)
    wide_factor = (WIDE_DIM + ROT_DIM) ** (-0.5)

    def start_state(count, width):
        return (
            jnp.full((count, row_count), -jnp.inf, jnp.float32),
            jnp.zeros((count, row_count), jnp.float32),
            jnp.zeros((row_count, count, width), jnp.float32),
        )

    carried = (start_state(narrow_dev, NARROW_DIM), start_state(wide_dev, WIDE_DIM))
    piece_keys = lax.all_gather(key_rows, "sp", axis=0, tiled=True)
    piece_rotary = lax.all_gather(rot_keys, "sp", axis=0, tiled=True)
    piece_values = lax.all_gather(value_rows, "sp", axis=0, tiled=True)
    length = piece_keys.shape[0]
    narrow_keys = piece_keys[:, :narrow_cols].reshape(length, narrow_dev, NARROW_DIM)
    wide_keys = piece_keys[:, narrow_cols:].reshape(length, wide_dev, WIDE_DIM)
    narrow_values = piece_values[:, :narrow_cols].reshape(length, narrow_dev, NARROW_DIM)
    wide_values = piece_values[:, narrow_cols:].reshape(length, wide_dev, WIDE_DIM)
    narrow_state = group_update(
        carried[0],
        query_narrow,
        rotary_narrow,
        narrow_keys,
        piece_rotary,
        narrow_values,
        narrow_factor,
    )
    wide_state = group_update(
        carried[1], query_wide, rotary_wide, wide_keys, piece_rotary, wide_values, wide_factor
    )
    narrow_state, wide_state = (narrow_state, wide_state)

    def finish(carried):
        return normalize(carried[2] / jnp.transpose(carried[1])[:, :, None]).reshape(row_count, -1)

    mixed = (
        jnp.concatenate([finish(narrow_state), finish(wide_state)], axis=1) * output_gain
    ).astype(jnp.bfloat16)
    whole_output = lax.all_gather(output_weight, "tp", axis=0, tiled=True)
    regrouped = lax.all_to_all(mixed, "tp", split_axis=0, concat_axis=1, tiled=True)
    projected = jnp.dot(regrouped, whole_output, preferred_element_type=jnp.float32)
    middle = (residual.astype(jnp.float32) + projected).astype(jnp.bfloat16)
    normed = (normalize(middle) * mixer_gain).astype(jnp.bfloat16)
    block_normed = lax.all_gather(normed, "tp", axis=0, tiled=True)
    gate_sums = jnp.dot(
        block_normed,
        lax.all_gather(gate_weight, "sp", axis=0, tiled=True),
        preferred_element_type=jnp.float32,
    )
    up_sums = jnp.dot(
        block_normed,
        lax.all_gather(up_weight, "sp", axis=0, tiled=True),
        preferred_element_type=jnp.float32,
    )
    down_whole = lax.all_gather(down_weight, "sp", axis=1, tiled=True)
    hidden = (jax.nn.silu(gate_sums) * up_sums).astype(jnp.bfloat16)
    channel_out = lax.psum_scatter(
        jnp.dot(hidden, down_whole, preferred_element_type=jnp.float32).astype(jnp.bfloat16),
        "tp",
        scatter_dimension=0,
        tiled=True,
    ).astype(jnp.float32)
    return (middle.astype(jnp.float32) + channel_out).astype(jnp.bfloat16)


MESH = pl.DeviceIdType.MESH
LANES = 128
PAIR = 2


def kernel(
    n_sp,
    query_ref,
    latent_ref,
    latent_gain_ref,
    key_weight_ref,
    value_weight_ref,
    output_gain_ref,
    mixer_gain_ref,
    cos_ref,
    sin_ref,
    swap_ref,
    residual_ref,
    output_weight_ref,
    gate_ref,
    up_ref,
    down_ref,
    turn_hbm,
    rotary_ref,
    out_ref,
    turn_ref,
    lat_all,
    rot_all,
    keys,
    values,
    res_all,
    out_all,
    mix_all,
    middle,
    normed,
    gate_all,
    up_all,
    down_all,
    hidden,
    part,
    from_core,
    to_x,
    from_x,
    to_z,
    from_z,
    summed_up,
    send_sems,
    recv_sems,
    local_sems,
):
    n_z = n_sp // PAIR
    s = lax.axis_index("sp")
    t = lax.axis_index("tp")
    z, y = s // PAIR, lax.rem(s, PAIR)
    x, c = t // PAIR, lax.rem(t, PAIR)
    rows, depth = latent_ref.shape
    half = rows // PAIR
    sibling = (s, x * PAIR + 1 - c)
    across = (s, (1 - x) * PAIR + c)
    beside = (z * PAIR + 1 - y, t)
    f32 = jnp.float32

    def z_id(step):
        return (lax.rem(z + step, n_z) * PAIR + y, t)

    barrier = pltpu.get_barrier_semaphore()
    greeted = [(lax.rem(s + k, n_sp), t) for k in range(1, n_sp)] + [sibling, across]
    for device in greeted:
        pl.semaphore_signal(barrier, inc=1, device_id=device, device_id_type=MESH)

    used = [0]
    locals_used = [0]
    sent = []

    def local(src, dst):
        copy = pltpu.make_async_copy(src, dst, local_sems.at[locals_used[0]])
        locals_used[0] += 1
        copy.start()
        return copy

    def send(src, dst, device):
        copy = pltpu.make_async_remote_copy(
            src_ref=src,
            dst_ref=dst,
            send_sem=send_sems.at[used[0]],
            recv_sem=recv_sems.at[used[0]],
            device_id=device,
            device_id_type=MESH,
        )
        used[0] += 1
        copy.start()
        sent.append(copy)
        return copy

    width = gate_all.shape[1]
    total_width = gate_ref.shape[1]
    slab = gate_ref.shape[0]

    def first(piece):
        return pl.multiple_of(jnp.minimum(piece * width, total_width - width), LANES)

    def span(owner):
        return pl.ds(pl.multiple_of(owner * slab, slab), slab)

    mine = span(s)
    my_piece = pl.ds(first(z), width)
    half_rows = pl.ds(pl.multiple_of(c * half, half), half)
    here = pl.ds(pl.multiple_of(s * rows, rows), rows)
    locals_first = [
        local(latent_ref, lat_all.at[here]),
        local(rotary_ref, rot_all.at[here]),
        local(turn_hbm, turn_ref),
    ]
    down_cols = pl.ds(pl.multiple_of(y * slab, slab), slab)
    locals_rest = [
        local(residual_ref, res_all.at[x, c, z]),
        local(output_weight_ref, out_all.at[x, c]),
        local(gate_ref.at[:, my_piece], gate_all.at[mine]),
        local(up_ref.at[:, my_piece], up_all.at[mine]),
        local(down_ref.at[my_piece], down_all.at[0, :, down_cols]),
    ]
    pl.semaphore_wait(barrier, len(greeted))

    def token_half(owner):
        return pl.ds(pl.multiple_of(owner * rows + c * half, half), half)

    def send_latent(device):
        return (
            send(latent_ref.at[half_rows], lat_all.at[token_half(s)], device),
            send(rotary_ref.at[half_rows], rot_all.at[token_half(s)], device),
        )

    def pass_latent(owner, device):
        place = token_half(owner)
        return (
            send(lat_all.at[place], lat_all.at[place], device),
            send(rot_all.at[place], rot_all.at[place], device),
        )

    def piece_of(step):
        return pl.ds(first(lax.rem(z + step, n_z)), width)

    latent_z = [send_latent(z_id(k)) for k in range(1, n_z)]
    latent_y = [send_latent(beside)]
    weight_x = send(output_weight_ref, out_all.at[x, c], across)
    gate_z = [
        send(gate_ref.at[:, piece_of(k)], gate_all.at[mine], z_id(k)) for k in range(1, n_z)
    ]
    z_far = lax.rem(z + PAIR, n_z)
    z_near = z + 1 - 2 * lax.rem(z, PAIR)
    near = (z_near * PAIR + y, t)
    residual_a = send(residual_ref, res_all.at[x, c, z], z_id(PAIR))

    latent_core = []
    for step in range(1, n_z):
        for copy in latent_z[step - 1]:
            copy.wait_recv()
        owner = lax.rem(z + n_z - step, n_z) * PAIR + y
        latent_y.append(pass_latent(owner, beside))
        latent_core.extend(pass_latent(owner, sibling))
    weight_y = [
        send(gate_ref.at[:, my_piece], gate_all.at[mine], beside),
        send(up_ref.at[:, my_piece], up_all.at[mine], beside),
        send(down_ref.at[my_piece], down_all.at[0, :, down_cols], beside),
    ]
    for step in range(n_z):
        for copy in latent_y[step]:
            copy.wait_recv()
        owner = lax.rem(z + n_z - step, n_z) * PAIR + 1 - y
        latent_core.extend(pass_latent(owner, sibling))
    weight_core = send(output_weight_ref, out_all.at[x, c], sibling)
    for copy in locals_first:
        copy.wait()
    for copy in latent_core:
        copy.wait_recv()

    gain = latent_gain_ref[...]

    def project(block, _):
        place = pl.ds(pl.multiple_of(block * rows, rows), rows)
        raw = lat_all[place, :].astype(f32)
        scale = lax.rsqrt(jnp.mean(raw * raw, axis=-1, keepdims=True) + epsilon)
        latent = (raw * scale * gain).astype(jnp.bfloat16)
        keys[place, :] = jnp.dot(latent, key_weight_ref[...], preferred_element_type=f32).astype(
            jnp.bfloat16
        )
        values[place, :] = jnp.dot(
            latent, value_weight_ref[...], preferred_element_type=f32
        ).astype(jnp.bfloat16)
        return 0

    lax.fori_loop(0, n_sp, project, 0)
    rot_width = rot_all.shape[1]
    rot_raw = rot_all[...]
    swap = swap_ref[...]
    rot_swapped = jnp.dot(rot_raw, swap[:rot_width, :rot_width], preferred_element_type=f32)
    rot_keys = (
        rot_raw.astype(f32) * cos_ref[:, :rot_width] + rot_swapped * sin_ref[:, :rot_width]
    ).astype(jnp.bfloat16)
    turn_raw = turn_ref[...]
    turn_swapped = jnp.dot(turn_raw, swap, preferred_element_type=f32)
    turned = (turn_raw.astype(f32) * cos_ref[here, :] + turn_swapped * sin_ref[here, :]).astype(
        jnp.bfloat16
    )

    content = query_ref.shape[1]
    head_count = turn_ref.shape[1] // rot_width
    wide_dev = (content - head_count * NARROW_DIM) // (WIDE_DIM - NARROW_DIM)
    sizes = [NARROW_DIM] * (head_count - wide_dev) + [WIDE_DIM] * wide_dev
    contract = (((1,), (1,)), ((), ()))
    heads = []
    start = 0
    for index, size in enumerate(sizes):
        cols = slice(start, start + size)
        scores = lax.dot_general(
            query_ref[:, cols], keys[:, cols], contract, preferred_element_type=f32
        )
        scores = scores + lax.dot_general(
            turned[:, index * rot_width : (index + 1) * rot_width],
            rot_keys,
            contract,
            preferred_element_type=f32,
        )
        scores = scores * (size + ROT_DIM) ** (-0.5)
        powers = jnp.exp(scores - jnp.max(scores, axis=-1, keepdims=True))
        totals = jnp.sum(powers, axis=-1, keepdims=True)
        summed = jnp.dot(
            powers.astype(jnp.bfloat16), values[:, cols], preferred_element_type=f32
        )
        attended = summed / totals
        scale = lax.rsqrt(jnp.mean(attended * attended, axis=-1, keepdims=True) + epsilon)
        heads.append(attended * scale)
        start += size
    mixed = (jnp.concatenate(heads, axis=1) * output_gain_ref[...]).astype(jnp.bfloat16)
    mix_all[x, c, z] = mixed

    mix_z = [send(mix_all.at[x, c, z], mix_all.at[x, c, z], z_id(k)) for k in range(1, n_z)]

    def relay(copies, buffer, step):
        copies[step - 1].wait_recv()
        block = buffer.at[span(lax.rem(z + n_z - step, n_z) * PAIR + y)]
        return send(block, block, beside)

    gate_y = [relay(gate_z, gate_all, k) for k in range(1, n_z)]
    residual_a.wait_recv()
    locals_rest[0].wait()
    residual_b = [
        send(res_all.at[x, c, block], res_all.at[x, c, block], near) for block in (z, z_far)
    ]
    up_z = [send(up_ref.at[:, piece_of(k)], up_all.at[mine], z_id(k)) for k in range(1, n_z)]
    down_z = [
        send(down_ref.at[piece_of(k)], down_all.at[k, :, down_cols], z_id(k))
        for k in range(1, n_z)
    ]

    for copy in locals_rest[1:]:
        copy.wait()
    weight_x.wait_recv()
    weight_far = send(out_all.at[1 - x, c], out_all.at[1 - x, c], sibling)
    for copy in mix_z:
        copy.wait_recv()
    mix_x = send(mix_all.at[x, c], mix_all.at[x, c], across)
    mix_core = send(mix_all.at[x, c], mix_all.at[x, c], sibling)
    for copy in residual_b:
        copy.wait_recv()
    residual_x = send(res_all.at[x, c], res_all.at[x, c], across)
    residual_core = send(res_all.at[x, c], res_all.at[x, c], sibling)
    mix_x.wait_recv()
    mix_far = send(mix_all.at[1 - x, c], mix_all.at[1 - x, c], sibling)
    up_y = [relay(up_z, up_all, 1)]
    residual_x.wait_recv()
    residual_far = send(res_all.at[1 - x, c], res_all.at[1 - x, c], sibling)
    up_y += [relay(up_z, up_all, k) for k in range(2, n_z)]
    for copy in (weight_core, weight_far, mix_core, mix_far, residual_core, residual_far):
        copy.wait_recv()

    mixer_gain = mixer_gain_ref[...]
    d_model = middle.shape[1]

    def finish_rows(block, _):
        place = pl.ds(pl.multiple_of(block * rows, rows), rows)
        total = res_all[:, :, block].reshape(rows, d_model).astype(f32)
        projected = jnp.zeros((rows, d_model), f32)
        for far in range(PAIR):
            for core in range(PAIR):
                projected = projected + jnp.dot(
                    mix_all[far, core, block], out_all[far, core], preferred_element_type=f32
                )
        mid = (total + projected).astype(jnp.bfloat16)
        middle[place, :] = mid
        wide = mid.astype(f32)
        scale = lax.rsqrt(jnp.mean(wide * wide, axis=-1, keepdims=True) + epsilon)
        normed[place, :] = (wide * scale * mixer_gain).astype(jnp.bfloat16)
        return 0

    lax.fori_loop(0, n_z, finish_rows, 0)

    def relay_down(step):
        down_z[step - 1].wait_recv()
        block = down_all.at[step, :, down_cols]
        return send(block, block, beside)

    down_y = [weight_y[2], relay_down(1)]
    for copy in gate_y + up_y + weight_y[:2]:
        copy.wait_recv()

    lane = lax.broadcasted_iota(jnp.int32, (rows, width), 1)
    fresh = lane + first(z) >= z * width

    def units(block, _):
        place = pl.ds(pl.multiple_of(block * rows, rows), rows)
        left = normed[place, :]
        gates = jnp.dot(left, gate_all[...], preferred_element_type=f32)
        ups = jnp.dot(left, up_all[...], preferred_element_type=f32)
        value = gates / (1.0 + jnp.exp(-gates)) * ups
        hidden[place, :] = jnp.where(fresh, value, 0.0).astype(jnp.bfloat16)
        return 0

    lax.fori_loop(0, n_z, units, 0)

    core_copies, x_copies, z_copies = [], [], []
    for step in range(n_z + 2):
        n = step - 2
        if 0 <= n < n_z:
            x_copies[n].wait_recv()
            to_z[n] = (to_x[n, :, x].astype(f32) + from_x[n].astype(f32)).astype(jnp.bfloat16)
            z_copies.append(
                [
                    send(to_z.at[n, lax.rem(z + k, n_z)], from_z.at[n, k - 1], z_id(k))
                    for k in range(1, n_z)
                ]
            )
        n = step - 1
        if 0 <= n < n_z:
            core_copies[n].wait_recv()
            to_x[n] = (part[n, :, :, c].astype(f32) + from_core[n].astype(f32)).astype(
                jnp.bfloat16
            )
            x_copies.append(send(to_x.at[n, :, 1 - x], from_x.at[n], across))
        n = step
        if n < n_z:
            if 2 <= n + 1 < n_z:
                down_y.append(relay_down(n + 1))
            down_y[n].wait_recv()
            product = jnp.dot(hidden[...], down_all[n], preferred_element_type=f32)
            part[n] = product.astype(jnp.bfloat16).reshape(part.shape[1:])
            core_copies.append(send(part.at[n, :, :, 1 - c], from_core.at[n], sibling))
    strip = out_ref.shape[0]
    chunk = part.shape[-1]
    own = pl.ds(pl.multiple_of(z * rows + t * strip, strip), strip)

    def cols_of(back):
        return pl.ds(pl.multiple_of(lax.rem(z + 2 * n_z - back, n_z) * chunk, chunk), chunk)

    for n in range(n_z):
        cols = cols_of(n)
        summed_up[:, cols] = middle[own, cols].astype(f32) + to_z[n, z].astype(f32)
    for n in range(n_z):
        for k in range(1, n_z):
            z_copies[n][k - 1].wait_recv()
            cols = cols_of(n + k)
            summed_up[:, cols] = summed_up[:, cols] + from_z[n, k - 1].astype(f32)
    out_ref[...] = summed_up[...].astype(jnp.bfloat16)
    for copy in sent:
        copy.wait_send()


def fused(
    n_sp,
    residual,
    query_content,
    query_rotary,
    key_latent,
    rotary_key,
    latent_gain,
    key_weight,
    value_weight,
    output_gain,
    output_weight,
    mixer_gain,
    gate_weight,
    up_weight,
    down_weight,
):
    n_z = n_sp // PAIR
    rows, latent_width = key_latent.shape
    strip, d_model = residual.shape
    tokens = rows * n_sp
    content = query_content.shape[1]
    turn_width = query_rotary.shape[1]
    half_width = ROT_DIM // 2
    inverse = np.float32(1.0) / np.power(
        np.float32(rope_base), np.arange(0, ROT_DIM, 2, dtype=np.float32) / np.float32(ROT_DIM)
    )
    angles = np.arange(tokens, dtype=np.float32)[:, None] * inverse[None, :].astype(np.float32)
    head_count = turn_width // ROT_DIM
    cosine = np.cos(angles).astype(np.float32)
    sine = np.sin(angles).astype(np.float32)
    cos_table = np.tile(np.concatenate([cosine, cosine], axis=1), (1, head_count))
    sin_table = np.tile(np.concatenate([-sine, sine], axis=1), (1, head_count))
    lane = np.arange(turn_width)
    other = lane // ROT_DIM * ROT_DIM + (lane + half_width) % ROT_DIM
    swap = np.zeros((turn_width, turn_width), np.float32)
    swap[other, lane] = 1.0
    tiles = gate_weight.shape[1] // LANES
    width = -(-tiles // n_z) * LANES
    slab = rows * n_z
    chunk = d_model // n_z
    bf16 = jnp.bfloat16
    n_copies = 4 * n_sp + 8 * n_z + 20 + n_z * (n_z + 1)
    vmem = pl.BlockSpec(memory_space=pltpu.VMEM)
    anywhere = pl.BlockSpec(memory_space=pl.ANY)
    return pl.pallas_call(
        functools.partial(kernel, n_sp),
        out_shape=jax.ShapeDtypeStruct((strip, d_model), bf16),
        in_specs=[vmem] * 10 + [anywhere] * 7,
        out_specs=vmem,
        scratch_shapes=[
            pltpu.VMEM((rows, turn_width), bf16),
            pltpu.VMEM((tokens, latent_width), bf16),
            pltpu.VMEM((tokens, ROT_DIM), bf16),
            pltpu.VMEM((tokens, content), bf16),
            pltpu.VMEM((tokens, content), bf16),
            pltpu.VMEM((PAIR, PAIR, n_z, strip, d_model), bf16),
            pltpu.VMEM((PAIR, PAIR, content, d_model), bf16),
            pltpu.VMEM((PAIR, PAIR, n_z, rows, content), bf16),
            pltpu.VMEM((slab, d_model), bf16),
            pltpu.VMEM((slab, d_model), bf16),
            pltpu.VMEM((d_model, width), bf16),
            pltpu.VMEM((d_model, width), bf16),
            pltpu.VMEM((n_z, width, chunk), bf16),
            pltpu.VMEM((slab, width), bf16),
            pltpu.VMEM((n_z, n_z, PAIR, PAIR, strip, chunk), bf16),
            pltpu.VMEM((n_z, n_z, PAIR, strip, chunk), bf16),
            pltpu.VMEM((n_z, n_z, PAIR, strip, chunk), bf16),
            pltpu.VMEM((n_z, n_z, strip, chunk), bf16),
            pltpu.VMEM((n_z, n_z, strip, chunk), bf16),
            pltpu.VMEM((n_z, n_z - 1, strip, chunk), bf16),
            pltpu.VMEM((strip, d_model), jnp.float32),
            pltpu.SemaphoreType.DMA((n_copies,)),
            pltpu.SemaphoreType.DMA((n_copies,)),
            pltpu.SemaphoreType.DMA((8,)),
        ],
        compiler_params=pltpu.CompilerParams(
            collective_id=0, has_side_effects=True, vmem_limit_bytes=60 * 1024 * 1024
        ),
        name="layer",
    )(
        query_content,
        key_latent,
        latent_gain.reshape(1, -1),
        key_weight,
        value_weight,
        output_gain.reshape(1, -1),
        mixer_gain.reshape(1, -1),
        jnp.asarray(cos_table),
        jnp.asarray(sin_table),
        jnp.asarray(swap, dtype=bf16),
        residual,
        output_weight,
        gate_weight,
        up_weight,
        down_weight,
        query_rotary,
        rotary_key,
    )


def solution(mesh):
    n_sp, n_tp = mesh.shape["sp"], mesh.shape["tp"]

    def program(*arrays):
        residual, gate_weight = arrays[0], arrays[11]
        fits = (
            n_tp == PAIR * PAIR
            and n_sp == PAIR**3
            and gate_weight.shape[0] * n_sp == residual.shape[1]
            and gate_weight.shape[0] % LANES == 0
            and gate_weight.shape[1] % LANES == 0
        )
        if fits:
            return fused(n_sp, *arrays)
        return on_device(*arrays)

    placed = (
        P(("sp", "tp"), None),
        P("sp", "tp"),
        P("sp", "tp"),
        P("sp", None),
        P("sp", None),
        P(),
        P(None, "tp"),
        P(None, "tp"),
        P("tp"),
        P("tp", None),
        P(),
        P("sp", "tp"),
        P("sp", "tp"),
        P("tp", "sp"),
    )
    return jax.shard_map(
        program, mesh=mesh, in_specs=placed, out_specs=P(("sp", "tp"), None), check_vma=False
    )
```

```python
import functools

import jax
import jax.numpy as jnp
import numpy as np
from jax import lax
from jax.experimental import pallas as pl
from jax.experimental.pallas import tpu as pltpu
from jax.sharding import PartitionSpec as P

NARROW_HEADS = 8
WIDE_HEADS = 4
NARROW_DIM = 64
WIDE_DIM = 128
ROT_DIM = 32


epsilon = 1e-06
rope_base = 500000.0


def normalize(values):
    values = values.astype(jnp.float32)
    return values * lax.rsqrt(jnp.mean(values * values, axis=-1, keepdims=True) + epsilon)


def rotate(values, positions):
    half_width = values.shape[-1] // 2
    inverse = 1.0 / jnp.power(
        rope_base, jnp.arange(0, 2 * half_width, 2, dtype=jnp.float32) / (2 * half_width)
    )
    angles = positions.astype(jnp.float32)[:, None] * inverse[None, :]
    table_shape = (angles.shape[0],) + (1,) * (values.ndim - 2) + (half_width,)
    cosine_table = jnp.cos(angles).reshape(table_shape)
    sine_table = jnp.sin(angles).reshape(table_shape)
    first_half = values[..., :half_width]
    second_half = values[..., half_width:]
    return jnp.concatenate(
        [
            first_half * cosine_table - second_half * sine_table,
            second_half * cosine_table + first_half * sine_table,
        ],
        axis=-1,
    )


def group_update(carried, query_part, rotary_part, key_part, rotary_keys, value_part, factor):
    running_max, totals, accumulated = carried
    scores = (
        jnp.einsum("qhd,khd->hqk", query_part, key_part, preferred_element_type=jnp.float32)
        + jnp.einsum("qhd,kd->hqk", rotary_part, rotary_keys, preferred_element_type=jnp.float32)
    ) * factor
    new_max = jnp.max(scores, axis=-1)
    shrink = jnp.exp(running_max - new_max)
    powers = jnp.exp(scores - new_max[..., None])
    totals = totals * shrink + jnp.sum(powers, axis=-1)
    added = jnp.einsum(
        "hqk,khd->qhd", powers.astype(jnp.bfloat16), value_part, preferred_element_type=jnp.float32
    )
    accumulated = accumulated * jnp.transpose(shrink)[:, :, None] + added
    return (new_max, totals, accumulated)


def on_device(
    residual,
    query_content,
    query_rotary,
    key_latent,
    rotary_key,
    latent_gain,
    key_weight,
    value_weight,
    output_gain,
    output_weight,
    mixer_gain,
    gate_weight,
    up_weight,
    down_weight,
):
    tp_count = lax.axis_size("tp")
    narrow_dev = NARROW_HEADS // tp_count
    wide_dev = WIDE_HEADS // tp_count
    row_count = key_latent.shape[0]
    positions = lax.axis_index("sp") * row_count + lax.iota(jnp.int32, row_count)
    latent = (normalize(key_latent) * latent_gain).astype(jnp.bfloat16)
    key_rows = jnp.dot(latent, key_weight, preferred_element_type=jnp.float32).astype(jnp.bfloat16)
    value_rows = jnp.dot(latent, value_weight, preferred_element_type=jnp.float32).astype(
        jnp.bfloat16
    )
    rot_keys = rotate(rotary_key.astype(jnp.float32), positions).astype(jnp.bfloat16)
    head_count = narrow_dev + wide_dev
    rot_queries = rotate(
        query_rotary.astype(jnp.float32).reshape(row_count, head_count, ROT_DIM), positions
    ).astype(jnp.bfloat16)
    narrow_cols = narrow_dev * NARROW_DIM
    query_narrow = query_content[:, :narrow_cols].reshape(row_count, narrow_dev, NARROW_DIM)
    query_wide = query_content[:, narrow_cols:].reshape(row_count, wide_dev, WIDE_DIM)
    rotary_narrow = rot_queries[:, :narrow_dev]
    rotary_wide = rot_queries[:, narrow_dev:]
    narrow_factor = (NARROW_DIM + ROT_DIM) ** (-0.5)
    wide_factor = (WIDE_DIM + ROT_DIM) ** (-0.5)

    def start_state(count, width):
        return (
            jnp.full((count, row_count), -jnp.inf, jnp.float32),
            jnp.zeros((count, row_count), jnp.float32),
            jnp.zeros((row_count, count, width), jnp.float32),
        )

    carried = (start_state(narrow_dev, NARROW_DIM), start_state(wide_dev, WIDE_DIM))
    piece_keys = lax.all_gather(key_rows, "sp", axis=0, tiled=True)
    piece_rotary = lax.all_gather(rot_keys, "sp", axis=0, tiled=True)
    piece_values = lax.all_gather(value_rows, "sp", axis=0, tiled=True)
    length = piece_keys.shape[0]
    narrow_keys = piece_keys[:, :narrow_cols].reshape(length, narrow_dev, NARROW_DIM)
    wide_keys = piece_keys[:, narrow_cols:].reshape(length, wide_dev, WIDE_DIM)
    narrow_values = piece_values[:, :narrow_cols].reshape(length, narrow_dev, NARROW_DIM)
    wide_values = piece_values[:, narrow_cols:].reshape(length, wide_dev, WIDE_DIM)
    narrow_state = group_update(
        carried[0],
        query_narrow,
        rotary_narrow,
        narrow_keys,
        piece_rotary,
        narrow_values,
        narrow_factor,
    )
    wide_state = group_update(
        carried[1], query_wide, rotary_wide, wide_keys, piece_rotary, wide_values, wide_factor
    )
    narrow_state, wide_state = (narrow_state, wide_state)

    def finish(carried):
        return normalize(carried[2] / jnp.transpose(carried[1])[:, :, None]).reshape(row_count, -1)

    mixed = (
        jnp.concatenate([finish(narrow_state), finish(wide_state)], axis=1) * output_gain
    ).astype(jnp.bfloat16)
    whole_output = lax.all_gather(output_weight, "tp", axis=0, tiled=True)
    regrouped = lax.all_to_all(mixed, "tp", split_axis=0, concat_axis=1, tiled=True)
    projected = jnp.dot(regrouped, whole_output, preferred_element_type=jnp.float32)
    middle = (residual.astype(jnp.float32) + projected).astype(jnp.bfloat16)
    normed = (normalize(middle) * mixer_gain).astype(jnp.bfloat16)
    block_normed = lax.all_gather(normed, "tp", axis=0, tiled=True)
    gate_sums = jnp.dot(
        block_normed,
        lax.all_gather(gate_weight, "sp", axis=0, tiled=True),
        preferred_element_type=jnp.float32,
    )
    up_sums = jnp.dot(
        block_normed,
        lax.all_gather(up_weight, "sp", axis=0, tiled=True),
        preferred_element_type=jnp.float32,
    )
    down_whole = lax.all_gather(down_weight, "sp", axis=1, tiled=True)
    hidden = (jax.nn.silu(gate_sums) * up_sums).astype(jnp.bfloat16)
    channel_out = lax.psum_scatter(
        jnp.dot(hidden, down_whole, preferred_element_type=jnp.float32).astype(jnp.bfloat16),
        "tp",
        scatter_dimension=0,
        tiled=True,
    ).astype(jnp.float32)
    return (middle.astype(jnp.float32) + channel_out).astype(jnp.bfloat16)


MESH = pl.DeviceIdType.MESH
LANES = 128
PAIR = 2


def kernel(
    n_sp,
    query_ref,
    latent_ref,
    latent_gain_ref,
    key_weight_ref,
    value_weight_ref,
    output_gain_ref,
    mixer_gain_ref,
    cos_ref,
    sin_ref,
    swap_ref,
    residual_ref,
    output_weight_ref,
    gate_ref,
    up_ref,
    down_ref,
    turn_hbm,
    rotary_ref,
    out_ref,
    turn_ref,
    lat_all,
    rot_all,
    keys,
    values,
    res_all,
    out_all,
    mix_all,
    middle,
    normed,
    gate_all,
    up_all,
    down_all,
    hidden,
    part,
    from_core,
    to_x,
    from_x,
    to_z,
    from_z,
    summed_up,
    send_sems,
    recv_sems,
    local_sems,
):
    n_z = n_sp // PAIR
    s = lax.axis_index("sp")
    t = lax.axis_index("tp")
    z, y = s // PAIR, lax.rem(s, PAIR)
    x, c = t // PAIR, lax.rem(t, PAIR)
    rows, depth = latent_ref.shape
    half = rows // PAIR
    sibling = (s, x * PAIR + 1 - c)
    across = (s, (1 - x) * PAIR + c)
    beside = (z * PAIR + 1 - y, t)
    f32 = jnp.float32

    def z_id(step):
        return (lax.rem(z + step, n_z) * PAIR + y, t)

    barrier = pltpu.get_barrier_semaphore()
    greeted = [(lax.rem(s + k, n_sp), t) for k in range(1, n_sp)] + [sibling, across]
    for device in greeted:
        pl.semaphore_signal(barrier, inc=1, device_id=device, device_id_type=MESH)

    used = [0]
    locals_used = [0]
    sent = []

    def local(src, dst):
        copy = pltpu.make_async_copy(src, dst, local_sems.at[locals_used[0]])
        locals_used[0] += 1
        copy.start()
        return copy

    def send(src, dst, device):
        copy = pltpu.make_async_remote_copy(
            src_ref=src,
            dst_ref=dst,
            send_sem=send_sems.at[used[0]],
            recv_sem=recv_sems.at[used[0]],
            device_id=device,
            device_id_type=MESH,
        )
        used[0] += 1
        copy.start()
        sent.append(copy)
        return copy

    width = gate_all.shape[1]
    total_width = gate_ref.shape[1]
    slab = gate_ref.shape[0]

    def first(piece):
        return pl.multiple_of(jnp.minimum(piece * width, total_width - width), LANES)

    def span(owner):
        return pl.ds(pl.multiple_of(owner * slab, slab), slab)

    mine = span(s)
    my_piece = pl.ds(first(z), width)
    half_rows = pl.ds(pl.multiple_of(c * half, half), half)
    here = pl.ds(pl.multiple_of(s * rows, rows), rows)
    locals_first = [
        local(latent_ref, lat_all.at[here]),
        local(rotary_ref, rot_all.at[here]),
        local(turn_hbm, turn_ref),
    ]
    down_cols = pl.ds(pl.multiple_of(y * slab, slab), slab)
    locals_rest = [
        local(residual_ref, res_all.at[x, c, z]),
        local(output_weight_ref, out_all.at[x, c]),
        local(gate_ref.at[:, my_piece], gate_all.at[mine]),
        local(up_ref.at[:, my_piece], up_all.at[mine]),
        local(down_ref.at[my_piece], down_all.at[0, :, down_cols]),
    ]
    pl.semaphore_wait(barrier, len(greeted))

    def token_half(owner):
        return pl.ds(pl.multiple_of(owner * rows + c * half, half), half)

    def send_latent(device):
        return (
            send(latent_ref.at[half_rows], lat_all.at[token_half(s)], device),
            send(rotary_ref.at[half_rows], rot_all.at[token_half(s)], device),
        )

    def pass_latent(owner, device):
        place = token_half(owner)
        return (
            send(lat_all.at[place], lat_all.at[place], device),
            send(rot_all.at[place], rot_all.at[place], device),
        )

    def piece_of(step):
        return pl.ds(first(lax.rem(z + step, n_z)), width)

    latent_z = [send_latent(z_id(k)) for k in range(1, n_z)]
    latent_y = [send_latent(beside)]
    weight_x = send(output_weight_ref, out_all.at[x, c], across)
    z_far = lax.rem(z + PAIR, n_z)
    z_near = z + 1 - 2 * lax.rem(z, PAIR)
    near = (z_near * PAIR + y, t)
    residual_a = send(residual_ref, res_all.at[x, c, z], z_id(PAIR))
    gate_z = [
        send(gate_ref.at[:, piece_of(k)], gate_all.at[mine], z_id(k)) for k in range(1, n_z)
    ]

    latent_core = []
    for step in range(1, n_z):
        for copy in latent_z[step - 1]:
            copy.wait_recv()
        owner = lax.rem(z + n_z - step, n_z) * PAIR + y
        latent_y.append(pass_latent(owner, beside))
        latent_core.extend(pass_latent(owner, sibling))
    weight_y = [
        send(gate_ref.at[:, my_piece], gate_all.at[mine], beside),
        send(up_ref.at[:, my_piece], up_all.at[mine], beside),
        send(down_ref.at[my_piece], down_all.at[0, :, down_cols], beside),
    ]
    residual_a.wait_recv()
    locals_rest[0].wait()
    residual_b = [
        send(res_all.at[x, c, block], res_all.at[x, c, block], near) for block in (z, z_far)
    ]
    for step in range(n_z):
        for copy in latent_y[step]:
            copy.wait_recv()
        owner = lax.rem(z + n_z - step, n_z) * PAIR + 1 - y
        latent_core.extend(pass_latent(owner, sibling))
    weight_core = send(output_weight_ref, out_all.at[x, c], sibling)
    for copy in locals_first:
        copy.wait()
    for copy in latent_core:
        copy.wait_recv()

    gain = latent_gain_ref[...]

    def project(block, _):
        place = pl.ds(pl.multiple_of(block * rows, rows), rows)
        raw = lat_all[place, :].astype(f32)
        scale = lax.rsqrt(jnp.mean(raw * raw, axis=-1, keepdims=True) + epsilon)
        latent = (raw * scale * gain).astype(jnp.bfloat16)
        keys[place, :] = jnp.dot(latent, key_weight_ref[...], preferred_element_type=f32).astype(
            jnp.bfloat16
        )
        values[place, :] = jnp.dot(
            latent, value_weight_ref[...], preferred_element_type=f32
        ).astype(jnp.bfloat16)
        return 0

    lax.fori_loop(0, n_sp, project, 0)
    rot_width = rot_all.shape[1]
    rot_raw = rot_all[...]
    swap = swap_ref[...]
    rot_swapped = jnp.dot(rot_raw, swap[:rot_width, :rot_width], preferred_element_type=f32)
    rot_keys = (
        rot_raw.astype(f32) * cos_ref[:, :rot_width] + rot_swapped * sin_ref[:, :rot_width]
    ).astype(jnp.bfloat16)
    turn_raw = turn_ref[...]
    turn_swapped = jnp.dot(turn_raw, swap, preferred_element_type=f32)
    turned = (turn_raw.astype(f32) * cos_ref[here, :] + turn_swapped * sin_ref[here, :]).astype(
        jnp.bfloat16
    )

    content = query_ref.shape[1]
    head_count = turn_ref.shape[1] // rot_width
    wide_dev = (content - head_count * NARROW_DIM) // (WIDE_DIM - NARROW_DIM)
    sizes = [NARROW_DIM] * (head_count - wide_dev) + [WIDE_DIM] * wide_dev
    contract = (((1,), (1,)), ((), ()))
    heads = []
    start = 0
    for index, size in enumerate(sizes):
        cols = slice(start, start + size)
        scores = lax.dot_general(
            query_ref[:, cols], keys[:, cols], contract, preferred_element_type=f32
        )
        scores = scores + lax.dot_general(
            turned[:, index * rot_width : (index + 1) * rot_width],
            rot_keys,
            contract,
            preferred_element_type=f32,
        )
        scores = scores * (size + ROT_DIM) ** (-0.5)
        powers = jnp.exp(scores - jnp.max(scores, axis=-1, keepdims=True))
        totals = jnp.sum(powers, axis=-1, keepdims=True)
        summed = jnp.dot(
            powers.astype(jnp.bfloat16), values[:, cols], preferred_element_type=f32
        )
        attended = summed / totals
        scale = lax.rsqrt(jnp.mean(attended * attended, axis=-1, keepdims=True) + epsilon)
        heads.append(attended * scale)
        start += size
    mixed = (jnp.concatenate(heads, axis=1) * output_gain_ref[...]).astype(jnp.bfloat16)
    mix_all[x, c, z] = mixed

    mix_z = [send(mix_all.at[x, c, z], mix_all.at[x, c, z], z_id(k)) for k in range(1, n_z)]

    up_z = [send(up_ref.at[:, piece_of(k)], up_all.at[mine], z_id(k)) for k in range(1, n_z)]
    down_z = [
        send(down_ref.at[piece_of(k)], down_all.at[k, :, down_cols], z_id(k))
        for k in range(1, n_z)
    ]

    def relay(copies, buffer, step):
        copies[step - 1].wait_recv()
        block = buffer.at[span(lax.rem(z + n_z - step, n_z) * PAIR + y)]
        return send(block, block, beside)

    gate_y = [relay(gate_z, gate_all, k) for k in range(1, n_z)]
    for copy in locals_rest[1:]:
        copy.wait()
    weight_x.wait_recv()
    weight_far = send(out_all.at[1 - x, c], out_all.at[1 - x, c], sibling)
    for copy in mix_z:
        copy.wait_recv()
    mix_x = send(mix_all.at[x, c], mix_all.at[x, c], across)
    mix_core = send(mix_all.at[x, c], mix_all.at[x, c], sibling)
    for copy in residual_b:
        copy.wait_recv()
    residual_x = send(res_all.at[x, c], res_all.at[x, c], across)
    residual_core = send(res_all.at[x, c], res_all.at[x, c], sibling)
    mix_x.wait_recv()
    mix_far = send(mix_all.at[1 - x, c], mix_all.at[1 - x, c], sibling)
    up_y = [relay(up_z, up_all, 1)]
    residual_x.wait_recv()
    residual_far = send(res_all.at[1 - x, c], res_all.at[1 - x, c], sibling)
    up_y += [relay(up_z, up_all, k) for k in range(2, n_z)]
    for copy in (weight_core, weight_far, mix_core, mix_far, residual_core, residual_far):
        copy.wait_recv()

    mixer_gain = mixer_gain_ref[...]
    d_model = middle.shape[1]

    def finish_rows(block, _):
        place = pl.ds(pl.multiple_of(block * rows, rows), rows)
        total = res_all[:, :, block].reshape(rows, d_model).astype(f32)
        projected = jnp.zeros((rows, d_model), f32)
        for far in range(PAIR):
            for core in range(PAIR):
                projected = projected + jnp.dot(
                    mix_all[far, core, block], out_all[far, core], preferred_element_type=f32
                )
        mid = (total + projected).astype(jnp.bfloat16)
        middle[place, :] = mid
        wide = mid.astype(f32)
        scale = lax.rsqrt(jnp.mean(wide * wide, axis=-1, keepdims=True) + epsilon)
        normed[place, :] = (wide * scale * mixer_gain).astype(jnp.bfloat16)
        return 0

    lax.fori_loop(0, n_z, finish_rows, 0)

    def relay_down(step):
        down_z[step - 1].wait_recv()
        block = down_all.at[step, :, down_cols]
        return send(block, block, beside)

    down_y = [weight_y[2], relay_down(1)]
    for copy in gate_y + up_y + weight_y[:2]:
        copy.wait_recv()

    lane = lax.broadcasted_iota(jnp.int32, (rows, width), 1)
    fresh = lane + first(z) >= z * width

    def units(block, _):
        place = pl.ds(pl.multiple_of(block * rows, rows), rows)
        left = normed[place, :]
        gates = jnp.dot(left, gate_all[...], preferred_element_type=f32)
        ups = jnp.dot(left, up_all[...], preferred_element_type=f32)
        value = gates / (1.0 + jnp.exp(-gates)) * ups
        hidden[place, :] = jnp.where(fresh, value, 0.0).astype(jnp.bfloat16)
        return 0

    lax.fori_loop(0, n_z, units, 0)

    core_copies, x_copies, z_copies = [], [], []
    for step in range(n_z + 2):
        n = step - 2
        if 0 <= n < n_z:
            x_copies[n].wait_recv()
            to_z[n] = (to_x[n, :, x].astype(f32) + from_x[n].astype(f32)).astype(jnp.bfloat16)
            z_copies.append(
                [
                    send(to_z.at[n, lax.rem(z + k, n_z)], from_z.at[n, k - 1], z_id(k))
                    for k in range(1, n_z)
                ]
            )
        n = step - 1
        if 0 <= n < n_z:
            core_copies[n].wait_recv()
            to_x[n] = (part[n, :, :, c].astype(f32) + from_core[n].astype(f32)).astype(
                jnp.bfloat16
            )
            x_copies.append(send(to_x.at[n, :, 1 - x], from_x.at[n], across))
        n = step
        if n < n_z:
            if 2 <= n + 1 < n_z:
                down_y.append(relay_down(n + 1))
            down_y[n].wait_recv()
            product = jnp.dot(hidden[...], down_all[n], preferred_element_type=f32)
            part[n] = product.astype(jnp.bfloat16).reshape(part.shape[1:])
            core_copies.append(send(part.at[n, :, :, 1 - c], from_core.at[n], sibling))
    strip = out_ref.shape[0]
    chunk = part.shape[-1]
    own = pl.ds(pl.multiple_of(z * rows + t * strip, strip), strip)

    def cols_of(back):
        return pl.ds(pl.multiple_of(lax.rem(z + 2 * n_z - back, n_z) * chunk, chunk), chunk)

    for n in range(n_z):
        cols = cols_of(n)
        summed_up[:, cols] = middle[own, cols].astype(f32) + to_z[n, z].astype(f32)
    for n in range(n_z):
        for k in range(1, n_z):
            z_copies[n][k - 1].wait_recv()
            cols = cols_of(n + k)
            summed_up[:, cols] = summed_up[:, cols] + from_z[n, k - 1].astype(f32)
    out_ref[...] = summed_up[...].astype(jnp.bfloat16)
    for copy in sent:
        copy.wait_send()


def fused(
    n_sp,
    residual,
    query_content,
    query_rotary,
    key_latent,
    rotary_key,
    latent_gain,
    key_weight,
    value_weight,
    output_gain,
    output_weight,
    mixer_gain,
    gate_weight,
    up_weight,
    down_weight,
):
    n_z = n_sp // PAIR
    rows, latent_width = key_latent.shape
    strip, d_model = residual.shape
    tokens = rows * n_sp
    content = query_content.shape[1]
    turn_width = query_rotary.shape[1]
    half_width = ROT_DIM // 2
    inverse = np.float32(1.0) / np.power(
        np.float32(rope_base), np.arange(0, ROT_DIM, 2, dtype=np.float32) / np.float32(ROT_DIM)
    )
    angles = np.arange(tokens, dtype=np.float32)[:, None] * inverse[None, :].astype(np.float32)
    head_count = turn_width // ROT_DIM
    cosine = np.cos(angles).astype(np.float32)
    sine = np.sin(angles).astype(np.float32)
    cos_table = np.tile(np.concatenate([cosine, cosine], axis=1), (1, head_count))
    sin_table = np.tile(np.concatenate([-sine, sine], axis=1), (1, head_count))
    lane = np.arange(turn_width)
    other = lane // ROT_DIM * ROT_DIM + (lane + half_width) % ROT_DIM
    swap = np.zeros((turn_width, turn_width), np.float32)
    swap[other, lane] = 1.0
    tiles = gate_weight.shape[1] // LANES
    width = -(-tiles // n_z) * LANES
    slab = rows * n_z
    chunk = d_model // n_z
    bf16 = jnp.bfloat16
    n_copies = 4 * n_sp + 8 * n_z + 20 + n_z * (n_z + 1)
    vmem = pl.BlockSpec(memory_space=pltpu.VMEM)
    anywhere = pl.BlockSpec(memory_space=pl.ANY)
    return pl.pallas_call(
        functools.partial(kernel, n_sp),
        out_shape=jax.ShapeDtypeStruct((strip, d_model), bf16),
        in_specs=[vmem] * 10 + [anywhere] * 7,
        out_specs=vmem,
        scratch_shapes=[
            pltpu.VMEM((rows, turn_width), bf16),
            pltpu.VMEM((tokens, latent_width), bf16),
            pltpu.VMEM((tokens, ROT_DIM), bf16),
            pltpu.VMEM((tokens, content), bf16),
            pltpu.VMEM((tokens, content), bf16),
            pltpu.VMEM((PAIR, PAIR, n_z, strip, d_model), bf16),
            pltpu.VMEM((PAIR, PAIR, content, d_model), bf16),
            pltpu.VMEM((PAIR, PAIR, n_z, rows, content), bf16),
            pltpu.VMEM((slab, d_model), bf16),
            pltpu.VMEM((slab, d_model), bf16),
            pltpu.VMEM((d_model, width), bf16),
            pltpu.VMEM((d_model, width), bf16),
            pltpu.VMEM((n_z, width, chunk), bf16),
            pltpu.VMEM((slab, width), bf16),
            pltpu.VMEM((n_z, n_z, PAIR, PAIR, strip, chunk), bf16),
            pltpu.VMEM((n_z, n_z, PAIR, strip, chunk), bf16),
            pltpu.VMEM((n_z, n_z, PAIR, strip, chunk), bf16),
            pltpu.VMEM((n_z, n_z, strip, chunk), bf16),
            pltpu.VMEM((n_z, n_z, strip, chunk), bf16),
            pltpu.VMEM((n_z, n_z - 1, strip, chunk), bf16),
            pltpu.VMEM((strip, d_model), jnp.float32),
            pltpu.SemaphoreType.DMA((n_copies,)),
            pltpu.SemaphoreType.DMA((n_copies,)),
            pltpu.SemaphoreType.DMA((8,)),
        ],
        compiler_params=pltpu.CompilerParams(
            collective_id=0, has_side_effects=True, vmem_limit_bytes=60 * 1024 * 1024
        ),
        name="layer",
    )(
        query_content,
        key_latent,
        latent_gain.reshape(1, -1),
        key_weight,
        value_weight,
        output_gain.reshape(1, -1),
        mixer_gain.reshape(1, -1),
        jnp.asarray(cos_table),
        jnp.asarray(sin_table),
        jnp.asarray(swap, dtype=bf16),
        residual,
        output_weight,
        gate_weight,
        up_weight,
        down_weight,
        query_rotary,
        rotary_key,
    )


def solution(mesh):
    n_sp, n_tp = mesh.shape["sp"], mesh.shape["tp"]

    def program(*arrays):
        residual, gate_weight = arrays[0], arrays[11]
        fits = (
            n_tp == PAIR * PAIR
            and n_sp == PAIR**3
            and gate_weight.shape[0] * n_sp == residual.shape[1]
            and gate_weight.shape[0] % LANES == 0
            and gate_weight.shape[1] % LANES == 0
        )
        if fits:
            return fused(n_sp, *arrays)
        return on_device(*arrays)

    placed = (
        P(("sp", "tp"), None),
        P("sp", "tp"),
        P("sp", "tp"),
        P("sp", None),
        P("sp", None),
        P(),
        P(None, "tp"),
        P(None, "tp"),
        P("tp"),
        P("tp", None),
        P(),
        P("sp", "tp"),
        P("sp", "tp"),
        P("tp", "sp"),
    )
    return jax.shard_map(
        program, mesh=mesh, in_specs=placed, out_specs=P(("sp", "tp"), None), check_vma=False
    )
```
